32 devices in a mesh: rep: 2 (over x), fs: 8 (over z, y), tp: 2 (over core).
Axes of the slice: x: 2, y: 2, z: 4, core: 2. Of those that a mesh axis runs over, the one named last changes fastest.
Arguments:
- tokens: bfloat16 [5120, 2048], P(('rep', 'fs')), may hold values from -6 to 6
- mixer_out: bfloat16 [5120, 2048], P(('rep', 'fs')), may hold values from -6 to 6
- gate_first: bfloat16 [2048, 2816], P('fs', 'tp'), may hold values from -0.125 to 0.125
- up_first: bfloat16 [2048, 2816], P('fs', 'tp'), may hold values from -0.125 to 0.125
- down_first: bfloat16 [2816, 2048], P('tp', 'fs'), may hold values from -0.3125 to 0.3125
- gate_second: bfloat16 [2048, 2816], P('fs', 'tp'), may hold values from -0.125 to 0.125
- up_second: bfloat16 [2048, 2816], P('fs', 'tp'), may hold values from -0.125 to 0.125
- down_second: bfloat16 [2816, 2048], P('tp', 'fs'), may hold values from -0.3125 to 0.3125
- gain_first: float32 [2048], replicated, may hold values from 0.1 to 1.9
- bias_first: float32 [2048], replicated, may hold values from -1.5 to 1.5
- gain_middle: float32 [2048], replicated, may hold values from 0.1 to 1.9
- bias_middle: float32 [2048], replicated, may hold values from -1.5 to 1.5
- gain_last: float32 [2048], replicated, may hold values from 0.1 to 1.9
- bias_last: float32 [2048], replicated, may hold values from -1.5 to 1.5
Outputs:
- layer_out: bfloat16 [5120, 2048], P(('rep', 'fs'))
The draws below stay inside these ranges and needn't reach their ends.
All inputs are finite; a program needn't handle non-finite values.
Results may differ from the reference program's by a relative error of at most 0.014.
Values may be sent and summed in bfloat16 or wider, within the bound.
A program may use at most 64 MiB of HBM per device.

```python
import math
import jax
import jax.numpy as jnp
from jax import lax

D = 2048
FF = 2816
TOKENS = 5120
N_TP = 2


def level_of(own_key, extent, shards, low, high):
    loudness, own = 1.0, jax.random.fold_in(own_key, 6)
    for axis_at, parts in shards:
        draws = jnp.exp(jax.random.uniform(jax.random.fold_in(own, axis_at), (parts,), jnp.float32, low / len(shards), high / len(shards)))
        loudness = loudness * jnp.repeat(draws, extent[axis_at] // parts).reshape([-1 if axis == axis_at else 1 for axis in range(len(extent))])
    return loudness


def normal_values(own_key, shape, width, bound, cuts=(), kind=jnp.bfloat16):
    result = width * jax.random.normal(own_key, shape, jnp.float32)
    if cuts:
        result = result * level_of(own_key, shape, cuts, -0.22, 0.18)
    return jnp.clip(result, -bound, bound).astype(kind)


def setup_inputs(seed: int = 0) -> dict:
    seeds = jax.random.split(jax.random.key(seed), 15)
    tokens = normal_values(seeds[0], (TOKENS, D), 1.0, 6.0, ((0, 16),))
    mixer_out = normal_values(seeds[1], (TOKENS, D), 1.0, 6.0, ((0, 16),))
    gate_first = normal_values(seeds[2], (D, FF), D ** -0.5, 0.125, ((0, 8), (1, 2)))
    up_first = normal_values(seeds[3], (D, FF), D ** -0.5, 0.125, ((0, 8), (1, 2)))
    down_first = normal_values(seeds[4], (FF, D), (FF // 8) ** -0.5, 0.3125, ((0, 2), (1, 8)))
    gate_second = normal_values(seeds[5], (D, FF), D ** -0.5, 0.125, ((0, 8), (1, 2)))
    up_second = normal_values(seeds[6], (D, FF), D ** -0.5, 0.125, ((0, 8), (1, 2)))
    down_second = normal_values(seeds[7], (FF, D), (FF // 8) ** -0.5, 0.3125, ((0, 2), (1, 8)))
    gain_first = jnp.clip(1.0 + 0.18 * jax.random.normal(seeds[8], (D,), jnp.float32), 0.1, 1.9)
    bias_first = normal_values(seeds[9], (D,), 0.3, 1.5, (), jnp.float32)
    gain_middle = jnp.clip(1.0 + 0.18 * jax.random.normal(seeds[10], (D,), jnp.float32), 0.1, 1.9)
    bias_middle = normal_values(seeds[11], (D,), 0.3, 1.5, (), jnp.float32)
    gain_last = jnp.clip(1.0 + 0.18 * jax.random.normal(seeds[12], (D,), jnp.float32), 0.1, 1.9)
    bias_last = normal_values(seeds[13], (D,), 0.3, 1.5, (), jnp.float32)
    return dict(tokens=tokens, mixer_out=mixer_out, gate_first=gate_first, up_first=up_first, down_first=down_first, gate_second=gate_second, up_second=up_second, down_second=down_second, gain_first=gain_first, bias_first=bias_first, gain_middle=gain_middle, bias_middle=bias_middle, gain_last=gain_last, bias_last=bias_last)


residual_scale = math.sqrt(2.0)
norm_eps = 1e-05

def normalize(summed, scaling, offset):
    center = summed - lax.optimization_barrier(jnp.mean(summed, axis=-1, keepdims=True))
    spread = lax.optimization_barrier(jnp.mean(center * center, axis=-1, keepdims=True))
    return center * lax.rsqrt(spread + norm_eps) * scaling.astype(jnp.float32) + offset.astype(jnp.float32)

def half_step(inputs, gate_weight, up_weight, down_weight):
    gate = jnp.dot(inputs, gate_weight, preferred_element_type=jnp.float32)
    value = jnp.dot(inputs, up_weight, preferred_element_type=jnp.float32)
    hidden = (jax.nn.silu(gate) * value).astype(jnp.bfloat16)
    block_size = hidden.shape[1] // N_TP
    running = jnp.zeros((inputs.shape[0], down_weight.shape[1]), jnp.float32)
    for member in range(N_TP):
        partial_value = jnp.dot(hidden[:, member * block_size:(member + 1) * block_size], down_weight[member * block_size:(member + 1) * block_size], preferred_element_type=jnp.float32)
        running = running + partial_value.astype(jnp.bfloat16).astype(jnp.float32)
    return running.astype(jnp.bfloat16)

def reference(tokens, mixer_out, gate_first, up_first, down_first, gate_second, up_second, down_second, gain_first, bias_first, gain_middle, bias_middle, gain_last, bias_last):
    first_branch = half_step(tokens, gate_first, up_first, down_first)
    first_norm = normalize(residual_scale * tokens.astype(jnp.float32) + 0.5 * first_branch.astype(jnp.float32), gain_first, bias_first).astype(jnp.bfloat16)
    middle_norm = normalize(residual_scale * first_norm.astype(jnp.float32) + mixer_out.astype(jnp.float32), gain_middle, bias_middle).astype(jnp.bfloat16)
    second_branch = half_step(middle_norm, gate_second, up_second, down_second)
    return normalize(residual_scale * middle_norm.astype(jnp.float32) + 0.5 * second_branch.astype(jnp.float32), gain_last, bias_last).astype(jnp.bfloat16)
```

```python
import functools
import math

import jax
import jax.numpy as jnp
from jax import lax
from jax.experimental import pallas as pl
from jax.experimental.pallas import tpu as pltpu
from jax.sharding import PartitionSpec as P

residual_scale = math.sqrt(2.0)
norm_eps = 1e-05
ZS, YS = 4, 2
F32, BF16 = jnp.float32, jnp.bfloat16


def normalize(summed, scaling, offset):
    center = summed - jnp.mean(summed, axis=-1, keepdims=True)
    spread = jnp.mean(center * center, axis=-1, keepdims=True)
    return center * lax.rsqrt(spread + norm_eps) * scaling + offset


def half_step(inputs, gate_weight, up_weight, down_weight):
    gate = jnp.dot(inputs, lax.all_gather(gate_weight, "fs", axis=0, tiled=True), preferred_element_type=F32)
    value = jnp.dot(inputs, lax.all_gather(up_weight, "fs", axis=0, tiled=True), preferred_element_type=F32)
    hidden = (jax.nn.silu(gate) * value).astype(BF16)
    partials = jnp.dot(hidden, lax.all_gather(down_weight, "fs", axis=1, tiled=True), preferred_element_type=F32)
    return lax.psum(partials.astype(BF16), "tp")


def per_device_general(
    tokens, mixer_out, gate_first, up_first, down_first, gate_second, up_second, down_second,
    gain_first, bias_first, gain_middle, bias_middle, gain_last, bias_last,
):
    first_branch = half_step(tokens, gate_first, up_first, down_first)
    first_norm = normalize(
        residual_scale * tokens.astype(F32) + 0.5 * first_branch.astype(F32), gain_first, bias_first
    ).astype(BF16)
    middle_norm = normalize(
        residual_scale * first_norm.astype(F32) + mixer_out.astype(F32), gain_middle, bias_middle
    ).astype(BF16)
    second_branch = half_step(middle_norm, gate_second, up_second, down_second)
    return normalize(
        residual_scale * middle_norm.astype(F32) + 0.5 * second_branch.astype(F32), gain_last, bias_last
    ).astype(BF16)


def slot(dz, dy):
    return (dz % ZS) * YS + dy % YS


SLOTS = ZS * YS
MESSAGES = {
    "a_p": ((1, 0), (0, 0), "A"),
    "a_m": ((-1, 0), (0, 0), "A"),
    "a_y": ((0, 1), (0, 0), "A"),
    "b_y": ((0, 1), (0, 0), "B"),
    "b_p": ((1, 0), (0, 0), "B"),
    "b_m": ((-1, 0), (0, 0), "B"),
    "a_pf": ((1, 0), (-1, 0), "A1"),
    "a_py": ((0, 1), (-1, 0), "A"),
    "a_mf": ((-1, 0), (1, 0), "A2"),
    "a_my": ((0, 1), (1, 0), "A"),
    "b_yp": ((1, 0), (0, 1), "B"),
    "b_ym": ((-1, 0), (0, 1), "B"),
    "b_mf": ((-1, 0), (1, 0), "B"),
    "a_pfy": ((0, 1), (-2, 0), "A1"),
    "a_mfy": ((0, 1), (2, 0), "A2"),
    "b_ypf": ((1, 0), (-1, 1), "B"),
}
NAMES = list(MESSAGES)


def row_parts(rows):
    a = (rows * 7 // 16) // 16 * 16
    a1 = (a // 2 + 15) // 16 * 16
    return {"A": (0, a), "A1": (0, a1), "A2": (a1, a - a1), "B": (a, rows - a)}


def kernel(
    tokens_ref, mixer_ref, gu1_ref, gu2_ref, d1_ref, d2_ref,
    g1_ref, b1_ref, g2_ref, b2_ref, g3_ref, b3_ref,
    out_ref,
    gu, dn, xb, acc, hid, keep, psend, precv, xsend, xrecv, br, mix, fin,
    wsend, wrecv, xs_send, xs_recv, ds_send, ds_recv, rs_send, rs_recv, local,
):
    rep, fs, core = lax.axis_index("rep"), lax.axis_index("fs"), lax.axis_index("tp")
    z, y = fs // YS, fs % YS
    quarter = fin.shape[0]
    half_hidden = dn.shape[2]
    ks = gu.shape[2]
    dcols = dn.shape[3]

    def fs_of(dz, dy):
        return lax.rem(z + dz + ZS, ZS) * YS + lax.rem(y + dy, YS)

    def plane(dz, dy):
        return {"fs": fs_of(dz, dy)}

    other_rep, other_core = {"rep": 1 - rep}, {"tp": 1 - core}
    mine = pl.ds(pl.multiple_of(core * quarter, quarter), quarter)
    sib = pl.ds(pl.multiple_of((1 - core) * quarter, quarter), quarter)

    hrows = pl.ds(pl.multiple_of(rep * half_hidden, half_hidden), half_hidden)
    own = slot(0, 0)
    loads = [
        pltpu.make_async_copy(gu1_ref, gu.at[0, own], local.at[0]),
        pltpu.make_async_copy(tokens_ref.at[mine], xb.at[0, pl.ds(0, quarter)], local.at[1]),
        pltpu.make_async_copy(tokens_ref.at[sib], xb.at[0, pl.ds(2 * quarter, quarter)], local.at[2]),
        pltpu.make_async_copy(d1_ref.at[hrows], dn.at[0, own], local.at[3]),
        pltpu.make_async_copy(gu2_ref, gu.at[1, own], local.at[4]),
        pltpu.make_async_copy(d2_ref.at[hrows], dn.at[1, own], local.at[5]),
        pltpu.make_async_copy(mixer_ref.at[mine], mix, local.at[6]),
    ]
    for load in loads:
        load.start()

    barrier = pltpu.get_barrier_semaphore()
    for target in (plane(1, 0), plane(-1, 0), plane(0, 1), other_rep, other_core):
        pl.semaphore_signal(barrier, inc=1, device_id=target, device_id_type=pl.DeviceIdType.MESH)
    pl.semaphore_wait(barrier, 5)

    sent = []

    def remote(src, dst, send_sem, recv_sem, target):
        return pltpu.make_async_remote_copy(
            src_ref=src, dst_ref=dst, send_sem=send_sem, recv_sem=recv_sem,
            device_id=target, device_id_type=pl.DeviceIdType.MESH,
        )

    def weight_copy(item, name):
        buf = (gu.at[0], dn.at[0], gu.at[1], dn.at[1])[item]
        (tz, ty), (bz, by), part = MESSAGES[name]
        start, size = row_parts(buf.shape[1])[part]
        rows = pl.ds(start, size)
        at = NAMES.index(name)
        return remote(
            buf.at[slot(bz, by), rows], buf.at[slot(bz - tz, by + ty), rows],
            wsend.at[item, at], wrecv.at[item, at], plane(tz, ty),
        )

    def send(copy):
        copy.start()
        sent.append(copy)

    def start(item, *names):
        for name in names:
            send(weight_copy(item, name))

    def arrived(item, *names):
        for name in names:
            weight_copy(item, name).wait_recv()

    def own_sends(item):
        loads[(0, 3, 4, 5)[item]].wait()
        start(item, "a_p", "a_m", "b_y", "a_y", "b_p", "b_m")

    def share_out(ffn):
        rows = pl.ds(0, quarter)
        send(remote(xb.at[ffn, rows], xb.at[ffn, pl.ds(quarter, quarter)],
                    xs_send.at[ffn], xs_recv.at[ffn], other_rep))

    def share_own(ffn):
        return remote(xb.at[ffn, pl.ds(0, quarter)], xb.at[ffn, pl.ds(2 * quarter, quarter)],
                      ds_send.at[ffn, 0], ds_recv.at[ffn, 0], other_core)

    def share_on(ffn):
        return remote(xb.at[ffn, pl.ds(quarter, quarter)], xb.at[ffn, pl.ds(3 * quarter, quarter)],
                      ds_send.at[ffn, 1], ds_recv.at[ffn, 1], other_core)

    def share_relay(ffn):
        remote(xb.at[ffn, pl.ds(0, quarter)], xb.at[ffn, pl.ds(quarter, quarter)],
               xs_send.at[ffn], xs_recv.at[ffn], other_rep).wait_recv()
        send(share_on(ffn))

    def share_done(ffn):
        if ffn:
            share_own(ffn).wait_recv()
        share_on(ffn).wait_recv()

    rows_step = 2 * quarter

    def gate_up(ffn, *offsets):
        for dz, dy in offsets:
            n = slot(dz, dy)
            cols = pl.ds(pl.multiple_of(fs_of(dz, dy) * ks, ks), ks)

            @pl.loop(0, 2)
            def _(i):
                rows = pl.ds(pl.multiple_of(i * rows_step, rows_step), rows_step)
                part = jnp.dot(xb[ffn, rows, cols], gu[ffn, n], preferred_element_type=F32)
                if n == own:
                    acc[rows, :] = part
                else:
                    acc[rows, :] += part

    def activate():
        low = half_hidden // 128 * 128
        wide = acc.shape[1] - low

        @pl.loop(0, 4 * quarter // 32)
        def _(i):
            rows = pl.ds(pl.multiple_of(i * 32, 32), 32)
            gate = acc[rows, :wide]
            value = acc[rows, low:]
            if half_hidden != low:
                value = pltpu.roll(value, wide - (half_hidden - low), axis=1)
            made = gate / (1.0 + jnp.exp(-gate)) * value
            hid[rows, :] = made[:, :half_hidden].astype(BF16)

    def to_sibling(ffn, n):
        return remote(psend.at[ffn, n], precv.at[ffn, n], rs_send.at[ffn, 0, n], rs_recv.at[ffn, 0, n], other_core)

    def to_pair(ffn, n):
        return remote(xsend.at[ffn, n], xrecv.at[ffn, n], rs_send.at[ffn, 1, n], rs_recv.at[ffn, 1, n], other_rep)

    def down(ffn, *offsets):
        for dz, dy in offsets:
            n = slot(dz, dy)
            whole = jnp.dot(hid[2 * quarter:, :], dn[ffn, n], preferred_element_type=F32)
            psend[ffn, n] = whole.astype(BF16)
            keep[n] = jnp.dot(hid[:2 * quarter, :], dn[ffn, n], preferred_element_type=F32)
            send(to_sibling(ffn, n))
        for dz, dy in offsets:
            n = slot(dz, dy)
            to_sibling(ffn, n).wait_recv()
            xsend[ffn, n] = (keep[n, quarter:, :] + precv[ffn, n, quarter:, :].astype(F32)).astype(BF16)
            keep[n, :quarter, :] = keep[n, :quarter, :] + precv[ffn, n, :quarter, :].astype(F32)
            send(to_pair(ffn, n))

    def collect(ffn, *offsets):
        for dz, dy in offsets:
            n = slot(dz, dy)
            to_pair(ffn, n).wait_recv()
            cols = pl.ds(pl.multiple_of(fs_of(dz, dy) * dcols, dcols), dcols)
            br[:, cols] = keep[n, :quarter, :] + xrecv[ffn, n].astype(F32)

    def first_norms():
        @pl.loop(0, quarter // 16)
        def _(i):
            rows = pl.ds(pl.multiple_of(i * 16, 16), 16)
            first = normalize(
                residual_scale * xb[0, rows, :].astype(F32) + 0.5 * br[rows, :], g1_ref[...], b1_ref[...]
            ).astype(BF16)
            xb[1, rows, :] = normalize(
                residual_scale * first.astype(F32) + mix[rows, :].astype(F32), g2_ref[...], b2_ref[...]
            ).astype(BF16)

    def last_norm():
        @pl.loop(0, quarter // 16)
        def _(i):
            rows = pl.ds(pl.multiple_of(i * 16, 16), 16)
            fin[rows, :] = normalize(
                residual_scale * xb[1, rows, :].astype(F32) + 0.5 * br[rows, :], g3_ref[...], b3_ref[...]
            ).astype(BF16)

    ready_1 = ((0, 1), (1, 0), (-1, 0))
    ready_2 = ((-1, 1), (1, 1))
    ready_3 = ((2, 0), (2, 1))

    for item in range(4):
        ffn = item // 2
        is_gu = item % 2 == 0
        step = functools.partial(gate_up if is_gu else down, ffn)
        if item == 0:
            own_sends(0)
            loads[1].wait()
            share_out(0)
        if item == 1:
            step((0, 0))
        if item == 3:
            step((0, 0))
        arrived(item, "a_p")
        start(item, "a_pf", "a_py")
        arrived(item, "a_m")
        start(item, "a_mf", "a_my")
        arrived(item, "b_y")
        start(item, "b_yp", "b_ym")
        if item == 2:
            collect(0, *ready_3)
            first_norms()
            share_out(1)
            send(share_own(1))
        arrived(item, "b_m")
        start(item, "b_mf")
        arrived(item, "b_p", "a_y")
        if item == 0:
            loads[2].wait()
            share_relay(0)
            share_done(0)
            step((0, 0))
        if item != 2:
            step(*ready_1)
        arrived(item, "a_pf")
        start(item, "a_pfy")
        arrived(item, "a_mf")
        start(item, "a_mfy")
        if item == 2:
            share_relay(1)
            share_done(1)
            step((0, 0), *ready_1)
        arrived(item, "b_yp")
        start(item, "b_ypf")
        arrived(item, "b_ym")
        if item < 3:
            own_sends(item + 1)
        arrived(item, "a_py", "a_my")
        step(*ready_2)
        if not is_gu:
            collect(ffn, (0, 0), *ready_1)
        arrived(item, "b_mf", "a_pfy", "a_mfy", "b_ypf")
        step(*ready_3)
        if is_gu:
            activate()
        else:
            collect(ffn, *ready_2)
            if item == 1:
                loads[6].wait()
    collect(1, *ready_3)
    last_norm()
    put = pltpu.make_async_copy(fin, out_ref.at[mine], local.at[7])
    put.start()
    over = remote(fin, out_ref.at[mine], ds_send.at[0, 0], ds_recv.at[0, 0], other_core)
    over.start()
    over.wait()
    put.wait()
    for copy in sent:
        copy.wait_send()


def per_device(
    tokens, mixer_out, gate_first, up_first, down_first, gate_second, up_second, down_second,
    gain_first, bias_first, gain_middle, bias_middle, gain_last, bias_last,
):
    rows, width = tokens.shape
    ks, hidden = gate_first.shape
    half_hidden = hidden // 2
    dcols = down_first.shape[1]
    quarter = rows // 2
    rep = lax.axis_index("rep")

    def own_half(gate, up):
        at = (0, rep * half_hidden)
        size = (ks, half_hidden)
        return jnp.concatenate([lax.dynamic_slice(gate, at, size), lax.dynamic_slice(up, at, size)], axis=1)

    any_spec, vmem = pl.BlockSpec(memory_space=pl.ANY), pl.BlockSpec(memory_space=pltpu.VMEM)
    vec = lambda v: v.reshape(1, width)
    dma = pltpu.SemaphoreType.DMA
    return pl.pallas_call(
        kernel,
        out_shape=jax.ShapeDtypeStruct((rows, width), BF16),
        in_specs=[any_spec] * 6 + [vmem] * 6,
        out_specs=any_spec,
        scratch_shapes=[
            pltpu.VMEM((2, SLOTS, ks, hidden), BF16),
            pltpu.VMEM((2, SLOTS, half_hidden, dcols), BF16),
            pltpu.VMEM((2, 4 * quarter, width), BF16),
            pltpu.VMEM((4 * quarter, hidden), F32),
            pltpu.VMEM((4 * quarter, half_hidden), BF16),
            pltpu.VMEM((SLOTS, 2 * quarter, dcols), F32),
            pltpu.VMEM((2, SLOTS, 2 * quarter, dcols), BF16),
            pltpu.VMEM((2, SLOTS, 2 * quarter, dcols), BF16),
            pltpu.VMEM((2, SLOTS, quarter, dcols), BF16),
            pltpu.VMEM((2, SLOTS, quarter, dcols), BF16),
            pltpu.VMEM((quarter, width), F32),
            pltpu.VMEM((quarter, width), BF16),
            pltpu.VMEM((quarter, width), BF16),
            dma((4, len(NAMES))), dma((4, len(NAMES))),
            dma((2,)), dma((2,)),
            dma((2, 2)), dma((2, 2)),
            dma((2, 2, SLOTS)), dma((2, 2, SLOTS)),
            dma((8,)),
        ],
        compiler_params=pltpu.CompilerParams(
            collective_id=0, has_side_effects=True, vmem_limit_bytes=60 * 1024 * 1024
        ),
    )(
        tokens, mixer_out, own_half(gate_first, up_first), own_half(gate_second, up_second),
        down_first, down_second,
        vec(gain_first), vec(bias_first), vec(gain_middle), vec(bias_middle), vec(gain_last), vec(bias_last),
    )


def on_mesh(mesh, rows, width, hidden):
    sizes = dict(mesh.shape)
    if (sizes["rep"], sizes["fs"], sizes["tp"]) != (2, SLOTS, 2):
        return False
    rows, ks, hidden = rows // (2 * SLOTS), width // SLOTS, hidden // 2
    return rows % 32 == 0 and ks % 128 == 0 and hidden % 128 == 0 and (hidden // 2) % 64 == 0


def solution(mesh):
    def run(tokens, mixer_out, gate_first, *rest):
        fits = on_mesh(mesh, tokens.shape[0], tokens.shape[1], gate_first.shape[1])
        return jax.shard_map(
            per_device if fits else per_device_general,
            mesh=mesh,
            in_specs=(
                P(("rep", "fs"), None), P(("rep", "fs"), None),
                P("fs", "tp"), P("fs", "tp"), P("tp", "fs"),
                P("fs", "tp"), P("fs", "tp"), P("tp", "fs"),
                P(), P(), P(), P(), P(), P(),
            ),
            out_specs=P(("rep", "fs"), None),
            check_vma=False,
        )(tokens, mixer_out, gate_first, *rest)

    return run
```

```python
import functools
import math

import jax
import jax.numpy as jnp
from jax import lax
from jax.experimental import pallas as pl
from jax.experimental.pallas import tpu as pltpu
from jax.sharding import PartitionSpec as P

residual_scale = math.sqrt(2.0)
norm_eps = 1e-05
ZS, YS = 4, 2
F32, BF16 = jnp.float32, jnp.bfloat16


def normalize(summed, scaling, offset):
    center = summed - jnp.mean(summed, axis=-1, keepdims=True)
    spread = jnp.mean(center * center, axis=-1, keepdims=True)
    return center * lax.rsqrt(spread + norm_eps) * scaling + offset


def half_step(inputs, gate_weight, up_weight, down_weight):
    gate = jnp.dot(inputs, lax.all_gather(gate_weight, "fs", axis=0, tiled=True), preferred_element_type=F32)
    value = jnp.dot(inputs, lax.all_gather(up_weight, "fs", axis=0, tiled=True), preferred_element_type=F32)
    hidden = (jax.nn.silu(gate) * value).astype(BF16)
    partials = jnp.dot(hidden, lax.all_gather(down_weight, "fs", axis=1, tiled=True), preferred_element_type=F32)
    return lax.psum(partials.astype(BF16), "tp")


def per_device_general(
    tokens, mixer_out, gate_first, up_first, down_first, gate_second, up_second, down_second,
    gain_first, bias_first, gain_middle, bias_middle, gain_last, bias_last,
):
    first_branch = half_step(tokens, gate_first, up_first, down_first)
    first_norm = normalize(
        residual_scale * tokens.astype(F32) + 0.5 * first_branch.astype(F32), gain_first, bias_first
    ).astype(BF16)
    middle_norm = normalize(
        residual_scale * first_norm.astype(F32) + mixer_out.astype(F32), gain_middle, bias_middle
    ).astype(BF16)
    second_branch = half_step(middle_norm, gate_second, up_second, down_second)
    return normalize(
        residual_scale * middle_norm.astype(F32) + 0.5 * second_branch.astype(F32), gain_last, bias_last
    ).astype(BF16)


def slot(dz, dy):
    return (dz % ZS) * YS + dy % YS


SLOTS = ZS * YS
STEPS = range(1, ZS)
NAMES = [("y", 0, 0), ("y", 1, 0)] + [
    (way, d, dy) for way in ("up", "dn", "xup", "xdn") for d in STEPS for dy in range(YS)
]


def kernel(
    tokens_ref, mixer_ref, gu1_ref, gu2_ref, d1_ref, d2_ref,
    g1_ref, b1_ref, g2_ref, b2_ref, g3_ref, b3_ref,
    out_ref,
    gu, dn, xb, acc, hid, keep, psend, precv, xsend, xrecv, br, mix, fin,
    wsend, wrecv, xs_send, xs_recv, ds_send, ds_recv, rs_send, rs_recv, local,
):
    rep, fs, core = lax.axis_index("rep"), lax.axis_index("fs"), lax.axis_index("tp")
    z, y = fs // YS, fs % YS
    quarter = fin.shape[0]
    half_hidden = dn.shape[2]
    ks = gu.shape[2]
    dcols = dn.shape[3]

    def fs_of(dz, dy):
        return lax.rem(z + dz + ZS, ZS) * YS + lax.rem(y + dy, YS)

    def plane(dz, dy):
        return {"fs": fs_of(dz, dy)}

    other_rep, other_core, pair = {"rep": 1 - rep}, {"tp": 1 - core}, plane(0, 1)
    mine = pl.ds(pl.multiple_of(core * quarter, quarter), quarter)
    sib = pl.ds(pl.multiple_of((1 - core) * quarter, quarter), quarter)

    def hrows(who):
        return pl.ds(pl.multiple_of(who * half_hidden, half_hidden), half_hidden)

    own = slot(0, 0)
    loads = [
        pltpu.make_async_copy(gu1_ref.at[y], gu.at[0, own], local.at[0]),
        pltpu.make_async_copy(tokens_ref.at[mine], xb.at[0, pl.ds(0, quarter)], local.at[1]),
        pltpu.make_async_copy(tokens_ref.at[sib], xb.at[0, pl.ds(2 * quarter, quarter)], local.at[2]),
        pltpu.make_async_copy(d1_ref.at[hrows(y)], dn.at[0, own], local.at[3]),
        pltpu.make_async_copy(gu2_ref.at[y], gu.at[1, own], local.at[4]),
        pltpu.make_async_copy(d2_ref.at[hrows(y)], dn.at[1, own], local.at[5]),
        pltpu.make_async_copy(mixer_ref.at[mine], mix, local.at[6]),
    ]
    for load in loads:
        load.start()

    barrier = pltpu.get_barrier_semaphore()

    def greet(target):
        pl.semaphore_signal(barrier, inc=1, device_id=target, device_id_type=pl.DeviceIdType.MESH)

    for target in (pair, other_rep, other_core):
        greet(target)

    @pl.when(z < ZS - 1)
    def _():
        greet(plane(1, 0))

    @pl.when(z > 0)
    def _():
        greet(plane(-1, 0))

    inner = jnp.logical_and(z > 0, z < ZS - 1)

    @pl.when(inner)
    def _():
        pl.semaphore_wait(barrier, 5)

    @pl.when(jnp.logical_not(inner))
    def _():
        pl.semaphore_wait(barrier, 4)

    sent = []

    def remote(src, dst, send_sem, recv_sem, target):
        return pltpu.make_async_remote_copy(
            src_ref=src, dst_ref=dst, send_sem=send_sem, recv_sem=recv_sem,
            device_id=target, device_id_type=pl.DeviceIdType.MESH,
        )

    def send(copy):
        copy.start()
        sent.append(copy)

    weights = (gu.at[0], dn.at[0], gu.at[1], dn.at[1])

    def weight_copy(item, name):
        way, d, dy = name
        buf = weights[item]
        rows = buf.shape[1] // 2
        part = pl.ds(pl.multiple_of(rep * rows, rows), rows)
        sems = wsend.at[item, NAMES.index(name)], wrecv.at[item, NAMES.index(name)]
        if way == "y":
            at = rep if d == 0 else 1 - rep
            part = pl.ds(pl.multiple_of(at * rows, rows), rows)
            if item % 2 == 0:
                src = (gu1_ref, None, gu2_ref)[item].at[1 - y, part]
            else:
                first = (1 - y) * half_hidden + at * rows
                src = (None, d1_ref, None, d2_ref)[item].at[pl.ds(pl.multiple_of(first, rows), rows)]
            return remote(src, buf.at[slot(0, 1), part], *sems, pair)
        sign = -1 if way in ("up", "xup") else 1
        there = buf.at[slot(sign * d, dy), part]
        if way in ("xup", "xdn"):
            return remote(there, there, *sems, other_rep)
        return remote(buf.at[slot(sign * (d - 1), dy), part], there, *sems, plane(-sign, 0))

    def sends_up(d):
        return jnp.logical_and(z >= d - 1, z < ZS - 1)

    def sends_dn(d):
        return jnp.logical_and(z + d - 1 <= ZS - 1, z > 0)

    def gets_up(d):
        return z >= d

    def gets_dn(d):
        return z + d <= ZS - 1

    def line_start(item, d, dy):
        @pl.when(sends_up(d))
        def _():
            weight_copy(item, ("up", d, dy)).start()

        @pl.when(sends_dn(d))
        def _():
            weight_copy(item, ("dn", d, dy)).start()

    def relay(item, d, dy):
        for way, gets in (("up", gets_up), ("dn", gets_dn)):
            @pl.when(gets(d))
            def _():
                weight_copy(item, (way, d, dy)).wait_recv()
                if d < ZS - 1:
                    @pl.when((sends_up if way == "up" else sends_dn)(d + 1))
                    def _():
                        weight_copy(item, (way, d + 1, dy)).start()
                weight_copy(item, ("x" + way, d, dy)).start()

    def swapped(item, d):
        for way, gets in (("xup", gets_up), ("xdn", gets_dn)):
            @pl.when(gets(d))
            def _():
                for dy in range(YS):
                    weight_copy(item, (way, d, dy)).wait_recv()

    def pair_start(item, part):
        send(weight_copy(item, ("y", part, 0)))

    def pair_wait(item, part):
        weight_copy(item, ("y", part, 0)).wait_recv()

    def share_out(ffn):
        return remote(xb.at[ffn, pl.ds(0, quarter)], xb.at[ffn, pl.ds(quarter, quarter)],
                      xs_send.at[ffn], xs_recv.at[ffn], pair)

    def share_own(ffn):
        return remote(xb.at[ffn, pl.ds(0, quarter)], xb.at[ffn, pl.ds(2 * quarter, quarter)],
                      ds_send.at[ffn, 0], ds_recv.at[ffn, 0], other_core)

    def share_on(ffn):
        return remote(xb.at[ffn, pl.ds(quarter, quarter)], xb.at[ffn, pl.ds(3 * quarter, quarter)],
                      ds_send.at[ffn, 1], ds_recv.at[ffn, 1], other_core)

    def share_finish(ffn):
        share_out(ffn).wait_recv()
        send(share_on(ffn))
        if ffn:
            share_own(ffn).wait_recv()
        share_on(ffn).wait_recv()

    rows_step = 2 * quarter

    def gate_up_slot(ffn, dz, dy, first=False):
        n = slot(dz, 0) + dy
        cols = pl.ds(pl.multiple_of(fs_of(dz, dy) * ks, ks), ks)

        @pl.loop(0, 2)
        def _(i):
            rows = pl.ds(pl.multiple_of(i * rows_step, rows_step), rows_step)
            part = jnp.dot(xb[ffn, rows, cols], gu[ffn, n], preferred_element_type=F32)
            if first:
                acc[rows, :] = part
            else:
                acc[rows, :] += part

    def at_distance(d, act):
        for dz, gets in ((-d, gets_up), (d, gets_dn)):
            @pl.when(gets(d))
            def _():
                @pl.loop(0, YS)
                def _(dy):
                    act(dz, dy)

    def activate():
        low = half_hidden // 128 * 128
        wide = acc.shape[1] - low

        @pl.loop(0, 4 * quarter // 32)
        def _(i):
            rows = pl.ds(pl.multiple_of(i * 32, 32), 32)
            gate = acc[rows, :wide]
            value = acc[rows, low:]
            if half_hidden != low:
                value = pltpu.roll(value, wide - (half_hidden - low), axis=1)
            made = gate / (1.0 + jnp.exp(-gate)) * value
            hid[rows, :] = made[:, :half_hidden].astype(BF16)

    def to_sibling(ffn, n):
        return remote(psend.at[ffn, n], precv.at[ffn, n], rs_send.at[ffn, 0, n], rs_recv.at[ffn, 0, n], other_core)

    def to_pair(ffn, dz, dy):
        n, there = slot(dz, 0) + dy, slot(dz, 0) + 1 - dy
        return remote(xsend.at[ffn, n], xrecv.at[ffn, there], rs_send.at[ffn, 1, n], rs_recv.at[ffn, 1, there], pair)

    def from_pair(ffn, n):
        return remote(xsend.at[ffn, n], xrecv.at[ffn, n], rs_send.at[ffn, 1, n], rs_recv.at[ffn, 1, n], pair)

    def down_slot(ffn, dz, dy):
        n = slot(dz, 0) + dy
        whole = jnp.dot(hid[2 * quarter:, :], dn[ffn, n], preferred_element_type=F32)
        psend[ffn, n] = whole.astype(BF16)
        keep[n] = jnp.dot(hid[:2 * quarter, :], dn[ffn, n], preferred_element_type=F32)
        to_sibling(ffn, n).start()

    def add_cores(ffn, dz, dy):
        n = slot(dz, 0) + dy
        to_sibling(ffn, n).wait_recv()
        xsend[ffn, n] = (keep[n, quarter:, :] + precv[ffn, n, quarter:, :].astype(F32)).astype(BF16)
        keep[n, :quarter, :] = keep[n, :quarter, :] + precv[ffn, n, :quarter, :].astype(F32)
        to_pair(ffn, dz, dy).start()

    def collect_slot(ffn, dz, dy):
        n = slot(dz, 0) + dy
        from_pair(ffn, n).wait_recv()
        cols = pl.ds(pl.multiple_of(fs_of(dz, dy) * dcols, dcols), dcols)
        br[:, cols] = keep[n, :quarter, :] + xrecv[ffn, n].astype(F32)

    def first_norms():
        @pl.loop(0, quarter // 16)
        def _(i):
            rows = pl.ds(pl.multiple_of(i * 16, 16), 16)
            first = normalize(
                residual_scale * xb[0, rows, :].astype(F32) + 0.5 * br[rows, :], g1_ref[...], b1_ref[...]
            ).astype(BF16)
            xb[1, rows, :] = normalize(
                residual_scale * first.astype(F32) + mix[rows, :].astype(F32), g2_ref[...], b2_ref[...]
            ).astype(BF16)

    def last_norm():
        @pl.loop(0, quarter // 16)
        def _(i):
            rows = pl.ds(pl.multiple_of(i * 16, 16), 16)
            fin[rows, :] = normalize(
                residual_scale * xb[1, rows, :].astype(F32) + 0.5 * br[rows, :], g3_ref[...], b3_ref[...]
            ).astype(BF16)

    def open_item(item):
        pair_start(item, 0)
        loads[(0, 3, 4, 5)[item]].wait()
        line_start(item, 1, 0)

    def second_start(item):
        pair_wait(item, 0)
        line_start(item, 1, 1)

    def work(item, d):
        ffn = item // 2
        if item % 2 == 0:
            at_distance(d, lambda dz, dy: gate_up_slot(ffn, dz, dy))
        else:
            at_distance(d, lambda dz, dy: down_slot(ffn, dz, dy))
            at_distance(d, lambda dz, dy: add_cores(ffn, dz, dy))

    def work_near(item, dy):
        ffn = item // 2
        if item % 2 == 0:
            gate_up_slot(ffn, 0, dy, first=dy == 0)
        else:
            down_slot(ffn, 0, dy)
            add_cores(ffn, 0, dy)

    def finish(item):
        ffn = item // 2
        for d in range(2, ZS):
            swapped(item, d)
            work(item, d)
        if item % 2 == 0:
            activate()
        else:
            for dy in range(YS):
                collect_slot(ffn, 0, dy)
            for d in STEPS:
                at_distance(d, lambda dz, dy: collect_slot(ffn, dz, dy))

    for item in range(4):
        if item == 0:
            open_item(0)
            loads[1].wait()
            send(share_out(0))
            pair_start(0, 1)
            second_start(0)
        relay(item, 1, 0)
        if item:
            finish(item - 1)
        if item == 2:
            loads[6].wait()
            first_norms()
            send(share_out(1))
            send(share_own(1))
            pair_start(2, 1)
        relay(item, 1, 1)
        if item == 0:
            loads[2].wait()
            share_finish(0)
        if item != 2:
            work_near(item, 0)
            pair_wait(item, 1)
            work_near(item, 1)
        for dy in range(YS):
            relay(item, 2, dy)
        if item < 3:
            open_item(item + 1)
            if item + 1 != 2:
                pair_start(item + 1, 1)
        if item == 2:
            share_finish(1)
            work_near(2, 0)
            pair_wait(2, 1)
            work_near(2, 1)
        relay(item, 3, 0)
        if item < 3:
            second_start(item + 1)
        swapped(item, 1)
        work(item, 1)
        relay(item, 3, 1)
    finish(3)
    last_norm()
    put = pltpu.make_async_copy(fin, out_ref.at[mine], local.at[7])
    put.start()
    over = remote(fin, out_ref.at[mine], ds_send.at[0, 0], ds_recv.at[0, 0], other_core)
    over.start()
    over.wait()
    put.wait()
    for copy in sent:
        copy.wait_send()
    for ffn in range(2):
        for n in range(SLOTS):
            to_sibling(ffn, n).wait_send()
            from_pair(ffn, n).wait_send()
    for item in range(4):
        for d in STEPS:
            for way, does in (("up", sends_up), ("dn", sends_dn), ("xup", gets_up), ("xdn", gets_dn)):
                @pl.when(does(d))
                def _():
                    for dy in range(YS):
                        weight_copy(item, (way, d, dy)).wait_send()


def per_device(
    tokens, mixer_out, gate_first, up_first, down_first, gate_second, up_second, down_second,
    gain_first, bias_first, gain_middle, bias_middle, gain_last, bias_last,
):
    rows, width = tokens.shape
    ks, hidden = gate_first.shape
    half_hidden = hidden // 2
    dcols = down_first.shape[1]
    quarter = rows // 2

    def halves(gate, up):
        return jnp.stack(
            [
                jnp.concatenate([w[:, at:at + half_hidden] for w in (gate, up)], axis=1)
                for at in (0, half_hidden)
            ]
        )

    any_spec, vmem = pl.BlockSpec(memory_space=pl.ANY), pl.BlockSpec(memory_space=pltpu.VMEM)
    vec = lambda v: v.reshape(1, width)
    dma = pltpu.SemaphoreType.DMA
    return pl.pallas_call(
        kernel,
        out_shape=jax.ShapeDtypeStruct((rows, width), BF16),
        in_specs=[any_spec] * 6 + [vmem] * 6,
        out_specs=any_spec,
        scratch_shapes=[
            pltpu.VMEM((2, SLOTS, ks, hidden), BF16),
            pltpu.VMEM((2, SLOTS, half_hidden, dcols), BF16),
            pltpu.VMEM((2, 4 * quarter, width), BF16),
            pltpu.VMEM((4 * quarter, hidden), F32),
            pltpu.VMEM((4 * quarter, half_hidden), BF16),
            pltpu.VMEM((SLOTS, 2 * quarter, dcols), F32),
            pltpu.VMEM((2, SLOTS, 2 * quarter, dcols), BF16),
            pltpu.VMEM((2, SLOTS, 2 * quarter, dcols), BF16),
            pltpu.VMEM((2, SLOTS, quarter, dcols), BF16),
            pltpu.VMEM((2, SLOTS, quarter, dcols), BF16),
            pltpu.VMEM((quarter, width), F32),
            pltpu.VMEM((quarter, width), BF16),
            pltpu.VMEM((quarter, width), BF16),
            dma((4, len(NAMES))), dma((4, len(NAMES))),
            dma((2,)), dma((2,)),
            dma((2, 2)), dma((2, 2)),
            dma((2, 2, SLOTS)), dma((2, 2, SLOTS)),
            dma((8,)),
        ],
        compiler_params=pltpu.CompilerParams(
            collective_id=0, has_side_effects=True, vmem_limit_bytes=60 * 1024 * 1024
        ),
    )(
        tokens, mixer_out, halves(gate_first, up_first), halves(gate_second, up_second),
        down_first, down_second,
        vec(gain_first), vec(bias_first), vec(gain_middle), vec(bias_middle), vec(gain_last), vec(bias_last),
    )


def on_mesh(mesh, rows, width, hidden):
    sizes = dict(mesh.shape)
    if (sizes["rep"], sizes["fs"], sizes["tp"]) != (2, SLOTS, 2):
        return False
    rows, ks, hidden = rows // (2 * SLOTS), width // SLOTS, hidden // 2
    return rows % 32 == 0 and ks % 128 == 0 and hidden % 128 == 0 and (hidden // 2) % 64 == 0


def solution(mesh):
    def run(tokens, mixer_out, gate_first, *rest):
        fits = on_mesh(mesh, tokens.shape[0], tokens.shape[1], gate_first.shape[1])
        return jax.shard_map(
            per_device if fits else per_device_general,
            mesh=mesh,
            in_specs=(
                P(("rep", "fs"), None), P(("rep", "fs"), None),
                P("fs", "tp"), P("fs", "tp"), P("tp", "fs"),
                P("fs", "tp"), P("fs", "tp"), P("tp", "fs"),
                P(), P(), P(), P(), P(), P(),
            ),
            out_specs=P(("rep", "fs"), None),
            check_vma=False,
        )(tokens, mixer_out, gate_first, *rest)

    return run
```
